32 devices in a mesh: ep: 8 (over z, y), tp: 4 (over x, core).
Axes of the slice: x: 2, y: 2, z: 4, core: 2. Of those that a mesh axis runs over, the one named last changes fastest.
Arguments:
- mix_input: bfloat16 [4096, 4096], P(('ep', 'tp')), may hold values from -30 to 30
- moe_input: bfloat16 [4096, 4096], P(('ep', 'tp')), may hold values from -6 to 6
- norm_mix: float32 [4096], replicated, may hold values from 0.1 to 1.9
- query_weight: bfloat16 [4096, 2048], P(None, 'tp'), may hold values from -0.09375 to 0.09375
- forget_weight: bfloat16 [4096, 2048], P(None, 'tp'), may hold values from -0.09375 to 0.09375
- value_weight: bfloat16 [4096, 2048], P(None, 'tp'), may hold values from -0.09375 to 0.09375
- forget_gap: float32 [2048], P('tp'), may hold values from 1e-05 to 0.06
- norm_out: float32 [2048], P('tp'), may hold values from 0.1 to 1.9
- norm_moe: float32 [4096], replicated, may hold values from 0.1 to 1.9
- router_weight: bfloat16 [4096, 8], replicated, may hold values from -0.09375 to 0.09375
- expert_gate: bfloat16 [8, 4096, 1024], P('ep', None, 'tp'), may hold values from -2 to 2, as said below
- expert_up: bfloat16 [8, 4096, 1024], P('ep', None, 'tp'), may hold values from -2 to 2, as said below
- expert_down: bfloat16 [8, 1024, 4096], P('ep', None, 'tp'), may hold values from -0.1875 to 0.1875
- routes: int32 [4096, 2], P('ep'), may hold values from 0 to 7, all different within a row; in each aligned block of 128 rows (0 to 127, 128 to 255, ...) at most 64 rows name the same one
Outputs:
- mixer_out: bfloat16 [4096, 2048], P('ep', 'tp')
- expert_out: bfloat16 [4096, 4096], P('ep', 'tp')
The draws below stay inside these ranges and needn't reach their ends.
Inputs may be any that keep to these rules, and one draw needn't show every extreme that they name: `routes`: each row names 2 different experts; in each aligned block of 128 rows no expert is named by more than 64 rows. `expert_gate`: independent entries, scaled by the fan-in 4096. `expert_up`: independent entries, scaled by the fan-in 4096.
All inputs are finite; a program needn't handle non-finite values.
Results may differ from the reference program's by a relative error of at most 0.012.
The reference program's roundings to bfloat16 on the way count: a program that leaves them out, or rounds other values in their place, can miss the bound.
Values may be sent and summed in bfloat16 or wider, within the bound.
A program may use at most 192 MiB of HBM per device.

```python
import math
import jax
import jax.numpy as jnp
import numpy as np
from jax import lax

D = 4096
HEADS = 16
HEAD_DIM = 128
HW = 2048
FF = 1024
EXPERTS = 8
TOPK = 2
BLOCK = 64
TOK_DEV = 128
TOKENS = 4096
CAP = 64


def draw_mix_input(key, part):
    noise_key, level_key, direction_key, scale_key = jax.random.split(jax.random.fold_in(key, 11), 4)
    block_total = TOKENS // TOK_DEV
    noise = jax.random.truncated_normal(noise_key, -6.0, 6.0, (TOKENS, D), jnp.float32)
    scale = jnp.ones((TOKENS, 1), jnp.float32)
    levels = jax.random.uniform(level_key, (block_total, 1), jnp.float32, -2.0, 2.0)
    direction = jax.random.truncated_normal(direction_key, -4.0, 4.0, (1, D), jnp.float32)
    row_values = noise + jnp.repeat(levels, TOK_DEV, axis=0) * direction
    return (row_values * scale).astype(jnp.bfloat16)


def draw_forget_gap(key, part):
    pick_key, slow_key, fast_key = jax.random.split(jax.random.fold_in(key, 23), 3)
    ordering = jax.random.permutation(pick_key, HEADS)
    slow_count = HEADS // 2
    slow = (ordering < slow_count)[:, None]
    slow_gap = jnp.exp(jax.random.uniform(slow_key, (HEADS, HEAD_DIM), jnp.float32, math.log(1e-05), math.log(0.0001)))
    fast_gap = jnp.exp(jax.random.uniform(fast_key, (HEADS, HEAD_DIM), jnp.float32, math.log(0.02), math.log(0.06)))
    return jnp.where(slow, slow_gap, fast_gap).reshape(HEADS * HEAD_DIM).astype(jnp.float32)


def expert_matrix(key):
    spread = 1.0
    entries = jax.random.truncated_normal(key, -6.0, 6.0, (EXPERTS, D, FF), jnp.float32)
    return (entries * (spread / math.sqrt(D))).astype(jnp.bfloat16)


def draw_expert_gate(key, part):
    return expert_matrix(jax.random.fold_in(key, 31))


def draw_expert_up(key, part):
    return expert_matrix(jax.random.fold_in(key, 37))


def block_scale(stream_key, shape, pieces, smallest, largest):
    loudness = 1.0
    for dim, shards_of in pieces:
        draws = jax.random.uniform(jax.random.fold_in(jax.random.fold_in(stream_key, 6), dim), (shards_of,), jnp.float32, smallest / len(pieces), largest / len(pieces))
        loudness = loudness * jnp.repeat(jnp.exp(draws), shape[dim] // shards_of).reshape((-1,) + (1,) * (len(shape) - 1 - dim))
    return loudness


def shared_out(stream_key, own, number, rows, amount, top, limit, slope):
    sequence = jax.random.permutation(stream_key, amount)
    crowded, ordinary = shares(amount, rows * top, limit, slope, True), shares(amount, rows * top, limit, slope, False)
    places = jnp.arange(amount)

    def named(lengths, offset_by):
        used = int((lengths > 0).sum())
        fixed = max(1, used // 4)
        moved = fixed + (places - fixed + offset_by * (used - fixed)) % max(1, amount - fixed)
        return jnp.zeros((amount,), jnp.int32).at[sequence[jnp.where(places < fixed, places, moved)]].set(jnp.asarray(lengths, jnp.int32))

    lengths = jnp.where(number % 4 == 0, named(crowded, number // 4), named(ordinary, number - number // 4 - 1))
    mixed = jax.random.permutation(jax.random.fold_in(own, 3), amount)
    giver, taker = mixed[0:amount // 2 * 2:2], mixed[1:amount // 2 * 2:2]
    room = jnp.minimum(lengths[giver] - 1, limit - lengths[taker]) // 2
    room = jnp.where((giver == sequence[0]) | (taker == sequence[0]) | (lengths[taker] == 0), 0, jnp.maximum(room, 0))
    moved = jax.random.randint(jax.random.fold_in(own, 4), (amount // 2,), 0, 1 << 20) % (room + 1)
    lengths = lengths.at[giver].add(-moved).at[taker].add(moved)
    items = jnp.searchsorted(jnp.cumsum(lengths), jnp.arange(rows * top), side="right").astype(jnp.int32)
    table = items.reshape(top, rows).T
    table = table[jax.random.permutation(jax.random.fold_in(own, 1), rows)]
    offset_by = jax.random.randint(jax.random.fold_in(own, 2), (rows, 1), 0, top)
    return jnp.take_along_axis(table, (jnp.arange(top)[None, :] + offset_by) % top, axis=1)


def shares(count, total, most, lean, full):
    weights = [(1 << 20) // math.isqrt(grade ** lean) + 1 for grade in range(1, count + 1)]
    largest = most if full else min(most, max(-(-total // count), total * weights[0] // sum(weights)))
    least = 1 if total - largest >= count - 1 else 0
    holding, surplus = [largest] + [least] * (count - 1), total - largest - least * (count - 1)
    while surplus > 0:
        free = [i for i in range(1, count) if holding[i] < largest] or [i for i in range(1, count) if holding[i] < most]
        whole, budget = sum([weights[i] for i in free]), surplus
        for i in free:
            addition = min(most - holding[i], max(1, budget * weights[i] // whole), surplus)
            holding[i] = holding[i] + addition
            surplus = surplus - addition
    return np.array(holding)


def bell_draw(key, dims, scale, reach, cuts=(), held_as=jnp.bfloat16):
    array = scale * jax.random.normal(key, dims, jnp.float32)
    if cuts:
        array = array * block_scale(key, dims, cuts, -0.22, 0.18)
    return jnp.clip(array, -reach, reach).astype(held_as)


def setup_inputs(seed: int = 0) -> dict:
    key_list = jax.random.split(jax.random.key(seed), 15)
    mix_input = draw_mix_input(jax.random.fold_in(key_list[14], 71), 0)
    moe_input = bell_draw(key_list[1], (TOKENS, D), 1.0, 6.0, ((0, 32),))
    norm_mix = jnp.clip(1.0 + 0.18 * jax.random.normal(key_list[2], (D,), jnp.float32), 0.1, 1.9)
    query_weight = bell_draw(key_list[3], (D, HW), D ** -0.5, 0.09375, ((1, 4),))
    forget_weight = bell_draw(key_list[4], (D, HW), D ** -0.5, 0.09375, ((1, 4),))
    value_weight = bell_draw(key_list[5], (D, HW), D ** -0.5, 0.09375, ((1, 4),))
    forget_gap = draw_forget_gap(jax.random.fold_in(key_list[14], 71), 0)
    norm_out = jnp.clip(1.0 + 0.18 * jax.random.normal(key_list[7], (HW,), jnp.float32), 0.1, 1.9)
    norm_moe = jnp.clip(1.0 + 0.18 * jax.random.normal(key_list[8], (D,), jnp.float32), 0.1, 1.9)
    router_weight = bell_draw(key_list[9], (D, EXPERTS), D ** -0.5, 0.09375)
    expert_gate = draw_expert_gate(jax.random.fold_in(key_list[14], 71), 0)
    expert_up = draw_expert_up(jax.random.fold_in(key_list[14], 71), 0)
    expert_down = bell_draw(key_list[12], (EXPERTS, FF, D), FF ** -0.5, 0.1875, ((0, 8), (2, 4)))
    routes_keys = jax.random.split(jax.random.fold_in(key_list[13], 1), TOKENS // TOK_DEV)
    routes_turns = jax.random.permutation(jax.random.fold_in(key_list[13], 3), TOKENS // TOK_DEV)
    routes = jax.vmap(lambda own, number: shared_out(jax.random.fold_in(key_list[13], 2), own, number, TOK_DEV, EXPERTS, TOPK, CAP, 1))(routes_keys, routes_turns).reshape((TOKENS, TOPK))
    return dict(mix_input=mix_input, moe_input=moe_input, norm_mix=norm_mix, query_weight=query_weight, forget_weight=forget_weight, value_weight=value_weight, forget_gap=forget_gap, norm_out=norm_out, norm_moe=norm_moe, router_weight=router_weight, expert_gate=expert_gate, expert_up=expert_up, expert_down=expert_down, routes=routes)


EPSILON = 1e-06
CLAMP_LIMIT = 7.0
SWISH_SLOPE = 1.702
MAXIMAL_ACCURACY = lax.Precision.HIGHEST

def normed(row_data, gain_vec):
    as_float = row_data.astype(jnp.float32)
    scale = lax.rsqrt(lax.optimization_barrier(jnp.mean(as_float * as_float, axis=-1, keepdims=True)) + EPSILON)
    return as_float * scale * gain_vec

def head_blocks(matrix, head_count):
    row_count = matrix.shape[0]
    return matrix.reshape(row_count // BLOCK, BLOCK, head_count, HEAD_DIM).transpose(0, 2, 1, 3)

def block_pass(running_state, inputs):
    query_rows, key_matrix_rows, value_rows, log_forget = inputs
    prefix_log_decay = jnp.cumsum(log_forget, axis=1)
    places = jnp.arange(BLOCK, dtype=jnp.int32)
    causal = (places[:, None] >= places[None, :])[None, :, :, None]
    spread = prefix_log_decay[:, :, None, :] - prefix_log_decay[:, None, :, :]
    decays = jnp.exp(jnp.where(causal, spread, -jnp.inf))
    scores = jnp.einsum('htk,hsk,htsk->hts', query_rows, key_matrix_rows, decays, precision=MAXIMAL_ACCURACY)
    inside = jnp.einsum('hts,hsv->htv', scores, value_rows, precision=MAXIMAL_ACCURACY)
    carried_state_block = jnp.einsum('faq,fqp->fap', query_rows * jnp.exp(prefix_log_decay), running_state, precision=MAXIMAL_ACCURACY)
    final_log_sum = prefix_log_decay[:, -1:, :]
    state_update = jnp.einsum('fge,fga->fea', key_matrix_rows * jnp.exp(final_log_sum - prefix_log_decay), value_rows, precision=MAXIMAL_ACCURACY)
    running_state = jnp.exp(final_log_sum[:, 0, :, None]) * running_state + state_update
    return (running_state, (inside + carried_state_block, prefix_log_decay))

def head_readout(block_out, gain_vec, head_count):
    block_total = block_out.shape[0]
    row_values = block_out.transpose(0, 2, 1, 3).reshape(block_total * BLOCK, head_count, HEAD_DIM)
    scale = lax.rsqrt(lax.optimization_barrier(jnp.mean(row_values * row_values, axis=-1, keepdims=True)) + EPSILON)
    shaped = row_values * scale * gain_vec.reshape(head_count, HEAD_DIM)
    return shaped.reshape(block_total * BLOCK, head_count * HEAD_DIM).astype(jnp.bfloat16)

def slot_places(routes, block_rows, expert_count, capacity):
    row_count = routes.shape[0]
    picks = routes.shape[1]
    flat_ids = routes.reshape(-1)
    onehot = (flat_ids[:, None] == jnp.arange(expert_count, dtype=jnp.int32)[None, :]).astype(jnp.int32)
    per_block = onehot.reshape(row_count // block_rows, block_rows * picks, expert_count)
    before = jnp.cumsum(per_block, axis=1) - per_block
    slot_rank = lax.optimization_barrier(jnp.sum(before * per_block, axis=2)).reshape(-1)
    anchor = jnp.arange(row_count * picks, dtype=jnp.int32) // (block_rows * picks)
    return (flat_ids * (row_count // block_rows) + anchor) * capacity + slot_rank

def route_weights(logits, routes):
    expert_count = logits.shape[1]
    chosen = routes[:, :, None] == jnp.arange(expert_count, dtype=jnp.int32)[None, None, :]
    picked = lax.optimization_barrier(jnp.sum(jnp.where(chosen, logits.astype(jnp.float32)[:, None, :], 0.0), axis=2))
    differences = picked[:, None, :] - picked[:, :, None]
    return 1.0 / lax.optimization_barrier(jnp.sum(jnp.exp(differences), axis=2))

def expert_rows(row_data, gate_mat, up_mat, down_mat):
    gate_pre = jnp.dot(row_data, gate_mat, preferred_element_type=jnp.float32)
    up_pre = jnp.dot(row_data, up_mat, preferred_element_type=jnp.float32)
    gated = jnp.minimum(gate_pre, CLAMP_LIMIT)
    opened = jnp.clip(up_pre, -CLAMP_LIMIT, CLAMP_LIMIT)
    hidden = ((opened + 1.0) * gated * jax.nn.sigmoid(SWISH_SLOPE * gated)).astype(jnp.bfloat16)
    return jnp.dot(hidden, down_mat, preferred_element_type=jnp.float32).astype(jnp.bfloat16)

def reference(mix_input, moe_input, norm_mix, query_weight, forget_weight, value_weight, forget_gap, norm_out, norm_moe, router_weight, expert_gate, expert_up, expert_down, routes):
    rows_a = normed(mix_input, norm_mix).astype(jnp.bfloat16)
    query_rows = jnp.dot(rows_a, query_weight, preferred_element_type=jnp.float32)
    forget_pre = jnp.dot(rows_a, forget_weight, preferred_element_type=jnp.float32)
    value_rows = jnp.dot(rows_a, value_weight, preferred_element_type=jnp.float32)
    shut = forget_gap * jax.nn.sigmoid(-forget_pre)
    log_forget = jnp.log1p(-shut)
    zero_state = jnp.zeros((HEADS, HEAD_DIM, HEAD_DIM), jnp.float32)
    end_state, (outputs, log_sums) = lax.scan(block_pass, zero_state, (head_blocks(query_rows, HEADS), head_blocks(shut, HEADS), head_blocks(value_rows, HEADS), head_blocks(log_forget, HEADS)))
    mixer_out = head_readout(outputs, norm_out, HEADS)
    rows_b = normed(moe_input, norm_moe).astype(jnp.bfloat16)
    logits = jnp.dot(rows_b, router_weight, preferred_element_type=jnp.float32).astype(jnp.bfloat16)
    weights = route_weights(logits, routes)
    block_total = TOKENS // TOK_DEV
    dest = slot_places(routes, TOK_DEV, EXPERTS, CAP)
    source = jnp.full((EXPERTS * block_total * CAP,), TOKENS, jnp.int32).at[dest].set(jnp.arange(TOKENS * TOPK, dtype=jnp.int32) // TOPK)
    padded = jnp.concatenate([rows_b, jnp.zeros((1, D), jnp.bfloat16)], axis=0)

    def one_expert(inputs):
        index_rows, gate_mat, up_mat, down_mat = inputs
        return expert_rows(padded[index_rows], gate_mat, up_mat, down_mat)
    results = lax.map(one_expert, (source.reshape(EXPERTS, block_total * CAP), expert_gate, expert_up, expert_down))
    flat_results = results.reshape(EXPERTS * block_total * CAP, D)
    dest_rows = dest.reshape(TOKENS, TOPK)
    total = jnp.zeros((TOKENS, D), jnp.float32)
    for slot_index in range(TOPK):
        total = total + weights[:, slot_index:slot_index + 1] * flat_results[dest_rows[:, slot_index]].astype(jnp.float32)
    expert_out = total.astype(jnp.bfloat16)
    return (mixer_out, expert_out)
```

```python
import functools

import jax
import jax.numpy as jnp
from jax import lax
from jax.experimental import pallas as pl
from jax.experimental.pallas import tpu as pltpu
from jax.sharding import PartitionSpec as P

HEAD_DIM = 128
CHUNK = 128
TOPK = 2
STATE_PAD = 8

EPSILON = 1e-06
CLAMP_LIMIT = 7.0
SWISH_SLOPE = 1.702
MAXIMAL_ACCURACY = lax.Precision.HIGHEST


def normed(row_data, gain_vec):
    as_float = row_data.astype(jnp.float32)
    scale = lax.rsqrt(jnp.mean(as_float * as_float, axis=-1, keepdims=True) + EPSILON)
    return (as_float * scale * gain_vec).astype(jnp.bfloat16)


def across(left, right, dims):
    return lax.dot_general(left, right, (dims, ((), ())), preferred_element_type=jnp.float32)


def halves(value):
    coarse = value.astype(jnp.bfloat16)
    return coarse, (value - coarse.astype(jnp.float32)).astype(jnp.bfloat16)


def split_product(left, right):
    left_a, left_b = halves(left)
    right_a, right_b = halves(right)
    dims = ((1,), (1,))
    return across(left_a, right_a, dims) + (across(left_a, right_b, dims) + across(left_b, right_a, dims))


def local_kernel(q_ref, f_ref, v_ref, gap_ref, inside_ref, decayed_ref, state_ref):
    rows = q_ref.shape[0]
    half = jnp.bfloat16
    down = lax.broadcasted_iota(jnp.int32, (CHUNK, CHUNK), 0)
    along = lax.broadcasted_iota(jnp.int32, (CHUNK, CHUNK), 1)
    causal = down >= along
    lower = causal.astype(jnp.float32)
    gap = gap_ref[...]
    state = jnp.zeros((HEAD_DIM, HEAD_DIM), jnp.float32)
    offset = jnp.zeros((1, HEAD_DIM), jnp.float32)
    for start in range(0, rows, CHUNK):
        here = pl.ds(start, CHUNK)
        shut = gap * jax.nn.sigmoid(-f_ref[here, :])
        log_forget = jnp.log1p(-shut)
        prefix = jnp.dot(lower, log_forget, precision=MAXIMAL_ACCURACY, preferred_element_type=jnp.float32)
        total = prefix[CHUNK - 1 : CHUNK, :]
        queries = q_ref[here, :] * jnp.exp(prefix)
        queries_half = queries.astype(half)
        queries_rest = (queries - queries_half.astype(jnp.float32)).astype(half)
        keys = (shut * jnp.exp(-prefix)).astype(half)
        ending = (shut * jnp.exp(total - prefix)).astype(half)
        values = v_ref[here, :]
        scores = across(queries_half, keys, ((1,), (1,))) + across(queries_rest, keys, ((1,), (1,)))
        inside = across(jnp.where(causal, scores, 0.0).astype(half), values, ((1,), (0,)))
        inside_ref[here, :] = inside + split_product(queries, state)
        decayed_ref[here, :] = queries * jnp.exp(offset)
        state = state * jnp.exp(total) + across(values, ending, ((0,), (0,)))
        offset = offset + total
    first = offset.astype(half)
    second = (offset - first.astype(jnp.float32)).astype(half)
    third = (offset - first.astype(jnp.float32) - second.astype(jnp.float32)).astype(half)
    coarse, rest = halves(state)
    state_ref[0, :HEAD_DIM, :] = coarse
    state_ref[0, HEAD_DIM : 2 * HEAD_DIM, :] = rest
    place = lax.broadcasted_iota(jnp.int32, (STATE_PAD, HEAD_DIM), 0)
    tail = jnp.where(
        place == 0,
        first.astype(jnp.float32),
        jnp.where(place == 1, second.astype(jnp.float32), jnp.where(place == 2, third.astype(jnp.float32), 0.0)),
    )
    state_ref[0, 2 * HEAD_DIM :, :] = tail.astype(half)


def local_pass(queries, forget_pre, values, gap):
    rows, width = queries.shape
    heads = width // HEAD_DIM
    column = pl.BlockSpec((rows, HEAD_DIM), lambda h: (0, h))
    return pl.pallas_call(
        local_kernel,
        grid=(heads,),
        in_specs=[column, column, column, pl.BlockSpec((1, HEAD_DIM), lambda h: (0, h))],
        out_specs=[
            column,
            column,
            pl.BlockSpec((1, 2 * HEAD_DIM + STATE_PAD, HEAD_DIM), lambda h: (h, 0, 0)),
        ],
        out_shape=[
            jax.ShapeDtypeStruct((rows, width), jnp.float32),
            jax.ShapeDtypeStruct((rows, width), jnp.float32),
            jax.ShapeDtypeStruct((heads, 2 * HEAD_DIM + STATE_PAD, HEAD_DIM), jnp.bfloat16),
        ],
        cost_estimate=pl.CostEstimate(flops=8_000_000_000, bytes_accessed=8_000_000, transcendentals=0),
        name="local_pass",
    )(queries, forget_pre, values, gap.reshape(1, width))


def arrive_kernel(here_ref, inside_ref, decayed_ref, states_ref, gain_ref, out_ref):
    here = here_ref[0]
    state = jnp.zeros((HEAD_DIM, HEAD_DIM), jnp.float32)
    for g in range(states_ref.shape[0] - 1):
        parts = states_ref[g, 0].astype(jnp.float32)
        total = jnp.sum(parts[2 * HEAD_DIM :], axis=0, keepdims=True)
        after = state * jnp.exp(total) + parts[:HEAD_DIM] + parts[HEAD_DIM : 2 * HEAD_DIM]
        state = jnp.where(g < here, after, state)
    readout = inside_ref[...] + split_product(decayed_ref[...], state)
    scale = lax.rsqrt(jnp.mean(readout * readout, axis=-1, keepdims=True) + EPSILON)
    out_ref[...] = (readout * scale * gain_ref[...]).astype(jnp.bfloat16)


def arrive_pass(here, inside, decayed, states, gain):
    rows, width = inside.shape
    heads = width // HEAD_DIM
    column = pl.BlockSpec((rows, HEAD_DIM), lambda h: (0, h))
    return pl.pallas_call(
        arrive_kernel,
        grid=(heads,),
        in_specs=[
            pl.BlockSpec(memory_space=pltpu.SMEM),
            column,
            column,
            pl.BlockSpec((states.shape[0], 1) + states.shape[2:], lambda h: (0, h, 0, 0)),
            pl.BlockSpec((1, HEAD_DIM), lambda h: (0, h)),
        ],
        out_specs=column,
        out_shape=jax.ShapeDtypeStruct((rows, width), jnp.bfloat16),
        cost_estimate=pl.CostEstimate(flops=4_000_000_000, bytes_accessed=8_000_000, transcendentals=0),
        name="arrive_pass",
    )(here.reshape(1), inside, decayed, states, gain.reshape(1, width))


def open_kernel(piece_count, *refs):
    pieces = refs[:piece_count]
    gate_ref, up_ref, out_ref, gate_sum, up_sum = refs[piece_count:]

    @pl.when(pl.program_id(1) == 0)
    def _():
        gate_sum[...] = jnp.zeros_like(gate_sum)
        up_sum[...] = jnp.zeros_like(up_sum)

    rows = jnp.concatenate([piece[0] for piece in pieces], axis=0)
    gate_sum[...] += jnp.dot(rows, gate_ref[0], preferred_element_type=jnp.float32)
    up_sum[...] += jnp.dot(rows, up_ref[0], preferred_element_type=jnp.float32)

    @pl.when(pl.program_id(1) == pl.num_programs(1) - 1)
    def _():
        gated = jnp.minimum(gate_sum[...], CLAMP_LIMIT)
        opened = jnp.clip(up_sum[...], -CLAMP_LIMIT, CLAMP_LIMIT)
        out_ref[0] = ((opened + 1.0) * gated * jax.nn.sigmoid(SWISH_SLOPE * gated)).astype(jnp.bfloat16)


def open_pass(pieces, gate_mat, up_mat):
    experts, rows, depth = pieces[0].shape
    width = gate_mat.shape[2]
    tile = depth // 4
    total_rows = rows * len(pieces)
    weight = pl.BlockSpec((1, tile, width), lambda e, k: (e, k, 0))
    return pl.pallas_call(
        functools.partial(open_kernel, len(pieces)),
        grid=(experts, depth // tile),
        in_specs=[pl.BlockSpec((1, rows, tile), lambda e, k: (e, 0, k))] * len(pieces) + [weight, weight],
        out_specs=pl.BlockSpec((1, total_rows, width), lambda e, k: (e, 0, 0)),
        out_shape=jax.ShapeDtypeStruct((experts, total_rows, width), jnp.bfloat16),
        scratch_shapes=[pltpu.VMEM((total_rows, width), jnp.float32)] * 2,
        cost_estimate=pl.CostEstimate(flops=5_000_000_000, bytes_accessed=9_000_000, transcendentals=0),
        name="open_pass",
    )(*pieces, gate_mat, up_mat)


def close_kernel(piece_count, chunk_count, *refs):
    pieces = refs[:piece_count]
    weight_ref = refs[piece_count]
    outs = refs[piece_count + 1 :]
    rows = pieces[0].shape[1] // piece_count
    slots = rows // chunk_count
    for block in range(piece_count):
        total = None
        for m in range(piece_count):
            at = (block ^ m) * rows
            part = jnp.dot(
                pieces[m][0, at : at + rows, :], weight_ref[0, m], preferred_element_type=jnp.float32
            )
            total = part if total is None else total + part
        total = total.astype(jnp.bfloat16)
        for c in range(chunk_count):
            outs[c][block, 0] = total[c * slots : (c + 1) * slots]


def close_pass(pieces, weight, chunk_count):
    experts, total_rows, depth = pieces[0].shape
    count = len(pieces)
    width = weight.shape[3]
    slots = total_rows // count // chunk_count
    tile = width // 2
    return pl.pallas_call(
        functools.partial(close_kernel, count, chunk_count),
        grid=(experts, width // tile),
        in_specs=[pl.BlockSpec((1, total_rows, depth), lambda e, n: (e, 0, 0))] * count
        + [pl.BlockSpec((1, count, depth, tile), lambda e, n: (e, 0, 0, n))],
        out_specs=[pl.BlockSpec((count, 1, slots, tile), lambda e, n: (0, e, 0, n))] * chunk_count,
        out_shape=[jax.ShapeDtypeStruct((count, experts, slots, width), jnp.bfloat16)] * chunk_count,
        cost_estimate=pl.CostEstimate(flops=3_000_000_000, bytes_accessed=5_000_000, transcendentals=0),
        name="close_pass",
    )(*pieces, weight)


def combine_kernel(place_ref, spread_ref, *refs):
    results, out_ref = refs[:-1], refs[-1]
    total = None
    for k, result in enumerate(results):
        part = jnp.dot(spread_ref[k, 0], result[0], preferred_element_type=jnp.float32)
        total = part if total is None else total + part
    out_ref[0] = total.astype(jnp.bfloat16)


def combine_pass(places, spread, results):
    count, blocks, rows, slots = spread.shape
    width = results[0].shape[2]
    return pl.pallas_call(
        combine_kernel,
        grid_spec=pltpu.PrefetchScalarGridSpec(
            num_scalar_prefetch=1,
            grid=(blocks,),
            in_specs=[pl.BlockSpec((count, 1, rows, slots), lambda m, p: (0, m, 0, 0))]
            + [pl.BlockSpec((1, slots, width), lambda m, p: (m, 0, 0))] * count,
            out_specs=pl.BlockSpec((1, rows, width), lambda m, p: (p[m], 0, 0)),
        ),
        out_shape=jax.ShapeDtypeStruct((blocks, rows, width), jnp.bfloat16),
        cost_estimate=pl.CostEstimate(flops=3_000_000_000, bytes_accessed=6_000_000, transcendentals=0),
        name="combine_pass",
    )(places, spread, *results)


def slot_ranks(routes, block_rows, expert_count):
    blocks = routes.reshape(-1, block_rows, routes.shape[1])
    named = blocks[..., None] == jnp.arange(expert_count, dtype=jnp.int32)
    per_row = jnp.sum(named, axis=2).astype(jnp.bfloat16)
    places = jnp.arange(block_rows)
    strict = (places[:, None] > places[None, :]).astype(jnp.bfloat16)
    before = jnp.einsum("ts,bse->bte", strict, per_row, preferred_element_type=jnp.float32)
    return jnp.sum(jnp.where(named, before[:, :, None, :], 0.0), axis=3).astype(jnp.int32)


def route_weights(logits, routes):
    expert_count = logits.shape[1]
    chosen = routes[:, :, None] == jnp.arange(expert_count, dtype=jnp.int32)[None, None, :]
    picked = jnp.sum(jnp.where(chosen, logits.astype(jnp.float32)[:, None, :], 0.0), axis=2)
    differences = picked[:, None, :] - picked[:, :, None]
    return 1.0 / jnp.sum(jnp.exp(differences), axis=2)


def swap(value, axis, mask):
    if mask == 0:
        return value
    count = lax.axis_size(axis)
    return lax.ppermute(value, axis, [(i, i ^ mask) for i in range(count)])


def spread_pieces(value, axis):
    pieces = [value]
    for m in range(1, lax.axis_size(axis)):
        low = m & -m
        pieces.append(swap(pieces[m ^ low], axis, low))
    return pieces


def per_device(
    mix_input,
    moe_input,
    norm_mix,
    query_weight,
    forget_weight,
    value_weight,
    forget_gap,
    norm_out,
    norm_moe,
    router_weight,
    expert_gate,
    expert_up,
    expert_down,
    routes,
):
    ep_count = lax.axis_size("ep")
    tp_count = lax.axis_size("tp")
    here = lax.axis_index("ep")
    own_index = lax.axis_index("tp")
    tok_dev = moe_input.shape[0]
    model_width = moe_input.shape[1]
    expert_count = router_weight.shape[1]
    local_experts = expert_gate.shape[0]
    capacity = 2 * tok_dev * TOPK // expert_count
    rows_b = normed(moe_input, norm_moe)
    ranks = slot_ranks(routes, tok_dev, expert_count)
    own_routes = lax.dynamic_slice_in_dim(routes, own_index * tok_dev, tok_dev, 0)
    own_ranks = lax.dynamic_index_in_dim(ranks, own_index, 0, keepdims=False)
    slots = jnp.arange(capacity, dtype=jnp.int32)
    locals_ = jnp.arange(local_experts, dtype=jnp.int32)

    def partner(k):
        return here ^ k

    def outgoing(k):
        expert = partner(k) * local_experts + locals_
        hits = (own_routes.T[None, None] == expert[:, None, None, None]) & (
            own_ranks.T[None, None] == slots[None, :, None, None]
        )
        select = jnp.any(hits, axis=2).astype(jnp.bfloat16)
        return jnp.einsum(
            "ect,td->ecd", select, rows_b, preferred_element_type=jnp.float32
        ).astype(jnp.bfloat16)

    quarter = max(1, ep_count // 4)
    spans = [list(range(s, min(s + quarter, ep_count))) for s in range(0, ep_count, quarter)]
    order = [spans[i] for i in (2, 0, 3, 1)] if len(spans) == 4 else spans
    ready = lax.optimization_barrier([outgoing(k) for k in range(ep_count)])
    received = {k: swap(ready[k], "ep", k) for span in order for k in span}

    rows_a = normed(mix_input, norm_mix)
    logits = jnp.dot(rows_b, router_weight, preferred_element_type=jnp.float32).astype(jnp.bfloat16)
    group_a = lax.all_gather(rows_a, "tp", axis=0, tiled=True)
    group_logits = lax.all_gather(logits, "tp", axis=0, tiled=True)
    query_rows = jnp.dot(group_a, query_weight, preferred_element_type=jnp.float32)
    forget_pre = jnp.dot(group_a, forget_weight, preferred_element_type=jnp.float32)
    value_rows = jnp.dot(group_a, value_weight, preferred_element_type=jnp.float32).astype(jnp.bfloat16)
    inside, decayed, own_state = local_pass(query_rows, forget_pre, value_rows, forget_gap)
    states = lax.all_gather(own_state, "ep")
    mixer_out = arrive_pass(here, inside, decayed, states, norm_out)

    places = own_index ^ jnp.arange(tp_count, dtype=jnp.int32)
    weights = route_weights(group_logits, routes).reshape(tp_count, tok_dev, TOPK)[places]
    block_routes = routes.reshape(tp_count, tok_dev, TOPK)[places]
    block_ranks = ranks[places]
    experts = (here ^ jnp.arange(ep_count, dtype=jnp.int32))[:, None] * local_experts + locals_
    targets = jnp.repeat(experts, capacity, axis=1)[:, None, None, :]
    slot_of = jnp.tile(slots, local_experts)
    spread = jnp.zeros((ep_count, tp_count, tok_dev, local_experts * capacity), jnp.float32)
    for j in range(TOPK):
        hits = (block_routes[None, :, :, j, None] == targets) & (block_ranks[None, :, :, j, None] == slot_of)
        spread = spread + jnp.where(hits, weights[None, :, :, j, None], 0.0)
    spread = spread.astype(jnp.bfloat16)
    down = expert_down.reshape(local_experts, tp_count, -1, expert_down.shape[2])
    down = jnp.take(down, places, axis=1)

    results = [None] * ep_count
    for span in order:
        block = jnp.stack([received[k] for k in span], axis=1)
        block = block.reshape(local_experts, len(span) * capacity, model_width)
        hidden = open_pass(spread_pieces(block, "tp"), expert_gate, expert_up)
        closed = close_pass(spread_pieces(hidden, "tp"), down, len(span))
        for k, result in zip(span, closed):
            back = swap(result, "ep", k)
            results[k] = back.reshape(tp_count, local_experts * capacity, back.shape[3])
    expert_out = combine_pass(places, spread, results).reshape(routes.shape[0], -1)
    return (mixer_out, expert_out)


def solution(mesh):
    return jax.shard_map(
        per_device,
        mesh=mesh,
        in_specs=(
            P(("ep", "tp"), None),
            P(("ep", "tp"), None),
            P(),
            P(None, "tp"),
            P(None, "tp"),
            P(None, "tp"),
            P("tp"),
            P("tp"),
            P(),
            P(),
            P("ep", None, "tp"),
            P("ep", None, "tp"),
            P("ep", None, "tp"),
            P("ep", None),
        ),
        out_specs=(P("ep", "tp"), P("ep", "tp")),
        check_vma=False,
    )
```
